32 devices in a mesh: rep: 2 (over x), fs: 8 (over z, y), tp: 2 (over core).
Axes of the slice: x: 2, y: 2, z: 4, core: 2. Of those that a mesh axis runs over, the one named last changes fastest.
Arguments:
- pre_gate: bfloat16 [12288, 4096], P(('rep', 'fs'), 'tp'), may hold values from -6 to 6
- pre_linear: bfloat16 [12288, 4096], P(('rep', 'fs'), 'tp'), may hold values from -6 to 6
- taps_gate: float32 [3, 4096], P(None, 'tp'), may hold values from -3.5 to 3.5
- taps_linear: float32 [3, 4096], P(None, 'tp'), may hold values from -3.5 to 3.5
- bias_gate: float32 [4096], P('tp'), may hold values from -3 to 3
- bias_linear: float32 [4096], P('tp'), may hold values from -3 to 3
- down_weight: bfloat16 [4096, 2048], P('tp', 'fs'), may hold values from -0.09375 to 0.09375
- out_grad: bfloat16 [12288, 2048], P(('rep', 'fs')), may hold values from -8 to 8
Outputs:
- grad_gate: bfloat16 [12288, 4096], P(('rep', 'fs'), 'tp')
- grad_linear: bfloat16 [12288, 4096], P(('rep', 'fs'), 'tp')
- grad_taps_gate: float32 [3, 4096], P(None, 'tp')
- grad_taps_linear: float32 [3, 4096], P(None, 'tp')
- grad_bias_gate: float32 [4096], P('tp')
- grad_bias_linear: float32 [4096], P('tp')
- grad_down: float32 [4096, 2048], P('tp', 'fs')
- row_norms: float32 [4096], P('tp')
The draws below stay inside these ranges and needn't reach their ends.
All inputs are finite; a program needn't handle non-finite values.
Results may differ from the reference program's by a relative error of at most 0.0031.
Values may be sent and summed in bfloat16 or wider, within the bound.
A program may use at most 128 MiB of HBM per device.

```python
import jax
import jax.numpy as jnp

D = 2048
FF = 4096
KERNEL = 3
TOK_DEV = 768
TOKENS = 12288


def raised(entries, key, source, target, blocks, factor):
    owner, partner = [(jnp.arange(entries.shape[axis_at]) // (entries.shape[axis_at] // blocks)).reshape([-1 if axis == axis_at else 1 for axis in range(entries.ndim)]) for axis_at in (source, target)]
    chosen = jax.random.permutation(key, blocks)[partner]
    strong = (owner == chosen) | (owner == (partner + blocks // 2) % blocks)
    return jnp.where(strong, factor * entries, entries)


def levels(rng, dims, cuts, low, high):
    gain, own = 1.0, jax.random.fold_in(rng, 6)
    for position, blocks in cuts:
        draws = jnp.exp(jax.random.uniform(jax.random.fold_in(own, position), (blocks,), jnp.float32, low / len(cuts), high / len(cuts)))
        gain = gain * jnp.repeat(draws, dims[position] // blocks).reshape([-1 if axis == position else 1 for axis in range(len(dims))])
    return gain


def bell_draw(own_key, shape, scale, limit, shards=(), kind=jnp.bfloat16):
    entries = scale * jax.random.normal(own_key, shape, jnp.float32)
    if shards:
        entries = entries * levels(own_key, shape, shards, -0.22, 0.18)
    return jnp.clip(entries, -limit, limit).astype(kind)


def heavy_noise(key, dims, deviation, most, pieces, heavy, kind=jnp.bfloat16):
    entries = deviation * jax.random.normal(key, dims, jnp.float32)
    if pieces:
        entries = entries * levels(key, dims, pieces, -0.22, 0.18)
    return jnp.clip(raised(entries, jax.random.fold_in(key, 3), *heavy), -most, most).astype(kind)


def setup_inputs(seed: int = 0) -> dict:
    seeds = jax.random.split(jax.random.key(seed), 9)
    return {
        "pre_gate": bell_draw(seeds[0], (TOKENS, FF), 1.0, 6.0, ((0, 16), (1, 2))),
        "pre_linear": bell_draw(seeds[1], (TOKENS, FF), 1.0, 6.0, ((0, 16), (1, 2))),
        "taps_gate": bell_draw(seeds[2], (KERNEL, FF), KERNEL ** -0.5, 3.5, ((1, 2),), jnp.float32),
        "taps_linear": bell_draw(seeds[3], (KERNEL, FF), KERNEL ** -0.5, 3.5, ((1, 2),), jnp.float32),
        "bias_gate": bell_draw(seeds[4], (FF,), 0.5, 3.0, ((0, 2),), jnp.float32),
        "bias_linear": bell_draw(seeds[5], (FF,), 0.5, 3.0, ((0, 2),), jnp.float32),
        "down_weight": bell_draw(seeds[6], (FF, D), FF ** -0.5, 0.09375, ((0, 2), (1, 8))),
        "out_grad": heavy_noise(seeds[7], (TOKENS, D), 1.0, 8.0, ((0, 16),), (0, 1, 16, 2.0)),
    }


def convolve(values, taps, bias):
    length = values.shape[1]
    padded = jnp.pad(values, ((0, 0), (2, 0), (0, 0)))
    return taps[0] * padded[:, 0:length] + taps[1] * padded[:, 1:length + 1] + taps[2] * padded[:, 2:length + 2] + bias


def convolve_back(grads, taps):
    length = grads.shape[1]
    padded = jnp.pad(grads, ((0, 0), (0, 2), (0, 0)))
    return taps[0] * padded[:, 2:length + 2] + taps[1] * padded[:, 1:length + 1] + taps[2] * padded[:, 0:length]


def tap_grads(grads, values):
    length = values.shape[1]
    padded = jnp.pad(values, ((0, 0), (2, 0), (0, 0)))
    return jnp.stack([jnp.sum(grads * padded[:, j:j + length], axis=(0, 1)) for j in range(3)])


def reference(pre_gate, pre_linear, taps_gate, taps_linear, bias_gate, bias_linear, down_weight, out_grad):
    seqs = pre_gate.shape[0] // TOK_DEV
    width = pre_gate.shape[1]
    gate_in = pre_gate.astype(jnp.float32).reshape(seqs, TOK_DEV, width)
    linear_in = pre_linear.astype(jnp.float32).reshape(seqs, TOK_DEV, width)
    gate_pre = convolve(gate_in, taps_gate, bias_gate)
    linear_pre = convolve(linear_in, taps_linear, bias_linear)
    sigma = jax.nn.sigmoid(gate_pre)
    silu_val = gate_pre * sigma
    hidden = (silu_val * linear_pre).astype(jnp.bfloat16).reshape(seqs * TOK_DEV, width)
    grad_hidden = jnp.dot(out_grad, down_weight.T, preferred_element_type=jnp.float32).reshape(seqs, TOK_DEV, width)
    grad_gate_pre = grad_hidden * linear_pre * sigma * (1.0 + gate_pre * (1.0 - sigma))
    grad_linear_pre = grad_hidden * silu_val
    grad_gate = convolve_back(grad_gate_pre, taps_gate).reshape(seqs * TOK_DEV, width).astype(jnp.bfloat16)
    grad_linear = convolve_back(grad_linear_pre, taps_linear).reshape(seqs * TOK_DEV, width).astype(jnp.bfloat16)
    grad_taps_gate = tap_grads(grad_gate_pre, gate_in)
    grad_taps_linear = tap_grads(grad_linear_pre, linear_in)
    grad_bias_gate = jnp.sum(grad_gate_pre, axis=(0, 1))
    grad_bias_linear = jnp.sum(grad_linear_pre, axis=(0, 1))
    grad_down = jnp.dot(hidden.T, out_grad, preferred_element_type=jnp.float32)
    row_norms = jnp.sum(grad_down * grad_down, axis=1)
    return (grad_gate, grad_linear, grad_taps_gate, grad_taps_linear, grad_bias_gate, grad_bias_linear, grad_down, row_norms)
```

```python
import functools

import jax
import jax.numpy as jnp
from jax import lax
from jax.experimental import pallas as pl
from jax.experimental.pallas import tpu as pltpu
from jax.sharding import PartitionSpec as P

MESH = pl.DeviceIdType.MESH


def shift_down(values, steps):
    if steps == 0:
        return values
    rows = lax.broadcasted_iota(jnp.int32, values.shape, 0)
    return jnp.where(rows < steps, 0.0, pltpu.roll(values, steps, 0))


def shift_up(values, steps):
    length = values.shape[0]
    rows = lax.broadcasted_iota(jnp.int32, values.shape, 0)
    return jnp.where(rows >= length - steps, 0.0, pltpu.roll(values, length - steps, 0))


def conv_chunk(values, taps, bias):
    return (
        taps[0:1] * shift_down(values, 2)
        + taps[1:2] * shift_down(values, 1)
        + taps[2:3] * values
        + bias
    )


def conv_back_chunk(grads, taps):
    return taps[0:1] * shift_up(grads, 2) + taps[1:2] * shift_up(grads, 1) + taps[2:3] * grads


def kernel(
    fs, chunk,
    pg_ref, pl_ref, tg_ref, tl_ref, bg_ref, bl_ref, w_ref, og_ref,
    gg_ref, gl_ref, cp_ref, gd_ref, rn_ref,
    wbuf, sbuf, rbuf, xs, xr, cpbuf, cps, cpx, rnbuf,
    w_send, w_recv, f_send, f_recv, s_send, s_recv, x_send, x_recv,
    c_send, c_recv, cx_send, cx_recv, n_send, n_recv,
):
    me = lax.axis_index("fs")
    rep = lax.axis_index("rep")
    partner = 1 - rep
    tokens, ff = pg_ref.shape
    dc = w_ref.shape[1]
    chunks = ff // chunk
    half = ff // 2
    per = -(-(fs - 1) // chunks)

    def to(k):
        return lax.rem(me + k, fs)

    def source(k):
        return lax.rem(me + fs - k, fs)

    def rows_of(c):
        return pl.ds(pl.multiple_of(c * chunk, chunk), chunk)

    def w_copy(k):
        rows = pl.ds(pl.multiple_of(rep * half, half), half)
        return pltpu.make_async_remote_copy(
            src_ref=w_ref.at[rows], dst_ref=wbuf.at[me, rows],
            send_sem=w_send.at[k], recv_sem=w_recv.at[k],
            device_id={"fs": to(k)}, device_id_type=MESH)

    def f_copy(k):
        rows = pl.ds(pl.multiple_of(rep * half, half), half)
        return pltpu.make_async_remote_copy(
            src_ref=wbuf.at[source(k), rows], dst_ref=wbuf.at[source(k), rows],
            send_sem=f_send.at[k], recv_sem=f_recv.at[k],
            device_id={"rep": partner}, device_id_type=MESH)

    def s_copy(c, k):
        return pltpu.make_async_remote_copy(
            src_ref=sbuf.at[to(k), rows_of(c)], dst_ref=rbuf.at[k, rows_of(c)],
            send_sem=s_send.at[c, k], recv_sem=s_recv.at[c, k],
            device_id={"fs": to(k)}, device_id_type=MESH)

    def x_copy(c):
        return pltpu.make_async_remote_copy(
            src_ref=xs.at[rows_of(c)], dst_ref=xr.at[rows_of(c)],
            send_sem=x_send.at[c], recv_sem=x_recv.at[c],
            device_id={"rep": partner}, device_id_type=MESH)

    def c_copy(k):
        return pltpu.make_async_remote_copy(
            src_ref=cpbuf.at[me], dst_ref=cpbuf.at[me],
            send_sem=c_send.at[k], recv_sem=c_recv.at[k],
            device_id={"fs": to(k)}, device_id_type=MESH)

    def cx_copy():
        return pltpu.make_async_remote_copy(
            src_ref=cps, dst_ref=cpx, send_sem=cx_send, recv_sem=cx_recv,
            device_id={"rep": partner}, device_id_type=MESH)

    def n_copy(k):
        return pltpu.make_async_remote_copy(
            src_ref=rnbuf.at[me], dst_ref=rnbuf.at[me],
            send_sem=n_send.at[k], recv_sem=n_recv.at[k],
            device_id={"fs": to(k)}, device_id_type=MESH)

    barrier = pltpu.get_barrier_semaphore()

    @pl.loop(1, fs)
    def _(k):
        pl.semaphore_signal(barrier, inc=1, device_id={"fs": to(k)}, device_id_type=MESH)

    pl.semaphore_signal(barrier, inc=1, device_id={"rep": partner}, device_id_type=MESH)
    pl.semaphore_wait(barrier, fs)

    @pl.loop(1, fs)
    def _(k):
        w_copy(k).start()

    wbuf[me] = w_ref[...]

    @pl.loop(0, chunks)
    def _(c):
        cols = rows_of(c)
        gate_pre = conv_chunk(
            pg_ref[:, cols].astype(jnp.float32), tg_ref[:, cols], bg_ref[:, cols])
        linear_pre = conv_chunk(
            pl_ref[:, cols].astype(jnp.float32), tl_ref[:, cols], bl_ref[:, cols])
        hidden = (gate_pre * jax.nn.sigmoid(gate_pre) * linear_pre).astype(jnp.bfloat16)
        for j in range(fs):
            part = lax.dot_general(
                hidden, og_ref[:, j * dc:(j + 1) * dc], (((0,), (0,)), ((), ())),
                preferred_element_type=jnp.float32)
            sbuf[j, cols] = part.astype(jnp.bfloat16)

        @pl.loop(1, fs)
        def _(k):
            s_copy(c, k).start()

        for step in range(per):
            k = c * per + step + 1

            @pl.when(k < fs)
            def _():
                w_copy(k).wait_recv()
                f_copy(k).start()

    @pl.loop(1, fs)
    def _(k):
        f_copy(k).wait_recv()

    @pl.loop(0, chunks)
    def _(c):
        cols = rows_of(c)
        gate_in = pg_ref[:, cols].astype(jnp.float32)
        linear_in = pl_ref[:, cols].astype(jnp.float32)
        taps_gate, taps_linear = tg_ref[:, cols], tl_ref[:, cols]
        gate_pre = conv_chunk(gate_in, taps_gate, bg_ref[:, cols])
        linear_pre = conv_chunk(linear_in, taps_linear, bl_ref[:, cols])
        sigma = jax.nn.sigmoid(gate_pre)
        grad_hidden = jnp.zeros((tokens, chunk), jnp.float32)
        for j in range(fs):
            grad_hidden += lax.dot_general(
                og_ref[:, j * dc:(j + 1) * dc], wbuf[j, cols], (((1,), (1,)), ((), ())),
                preferred_element_type=jnp.float32)
        grad_gate_pre = grad_hidden * linear_pre * sigma * (1.0 + gate_pre * (1.0 - sigma))
        grad_linear_pre = grad_hidden * (gate_pre * sigma)
        gg_ref[:, cols] = conv_back_chunk(grad_gate_pre, taps_gate).astype(jnp.bfloat16)
        gl_ref[:, cols] = conv_back_chunk(grad_linear_pre, taps_linear).astype(jnp.bfloat16)
        for j in range(3):
            cpbuf[me, j:j + 1, cols] = jnp.sum(
                grad_gate_pre * shift_down(gate_in, 2 - j), axis=0, keepdims=True)
            cpbuf[me, j + 3:j + 4, cols] = jnp.sum(
                grad_linear_pre * shift_down(linear_in, 2 - j), axis=0, keepdims=True)
        cpbuf[me, 6:7, cols] = jnp.sum(grad_gate_pre, axis=0, keepdims=True)
        cpbuf[me, 7:8, cols] = jnp.sum(grad_linear_pre, axis=0, keepdims=True)

        @pl.when(c == chunks - 1)
        def _():
            @pl.loop(1, fs)
            def _(k):
                c_copy(k).start()

        total = sbuf[me, cols].astype(jnp.float32)
        for k in range(1, fs):
            s_copy(c, k).wait_recv()
            total += rbuf[k, cols].astype(jnp.float32)
        xs[cols] = total
        x_copy(c).start()

    @pl.loop(1, fs)
    def _(k):
        c_copy(k).wait_recv()

    sums = cpbuf[0]
    for j in range(1, fs):
        sums += cpbuf[j]
    cps[...] = sums
    cx_copy().start()

    @pl.loop(0, chunks)
    def _(c):
        rows = rows_of(c)
        x_copy(c).wait_recv()
        total = xs[rows] + xr[rows]
        gd_ref[rows] = total
        square = total * total
        while square.shape[1] % 256 == 0:
            middle = square.shape[1] // 2
            square = square[:, :middle] + square[:, middle:]
        rnbuf[me, 0:1, rows] = jnp.sum(square.T, axis=0, keepdims=True)

    @pl.loop(1, fs)
    def _(k):
        n_copy(k).start()

    cx_copy().wait_recv()
    cp_ref[...] = cps[...] + cpx[...]

    @pl.loop(1, fs)
    def _(k):
        n_copy(k).wait_recv()

    norms = rnbuf[0]
    for j in range(1, fs):
        norms += rnbuf[j]
    rn_ref[...] = norms

    cx_copy().wait_send()

    @pl.loop(1, fs)
    def _(k):
        w_copy(k).wait_send()
        f_copy(k).wait_send()
        c_copy(k).wait_send()
        n_copy(k).wait_send()

    @pl.loop(0, chunks)
    def _(c):
        x_copy(c).wait_send()

        @pl.loop(1, fs)
        def _(k):
            s_copy(c, k).wait_send()


def local(
    fs, pre_gate, pre_linear, taps_gate, taps_linear, bias_gate, bias_linear, down_weight, out_grad
):
    tokens, ff = pre_gate.shape
    dc = down_weight.shape[1]
    chunk = 256
    chunks = ff // chunk
    f32, bf16 = jnp.float32, jnp.bfloat16
    vmem = pl.BlockSpec(memory_space=pltpu.VMEM)
    dma = pltpu.SemaphoreType.DMA
    gg, gl, cp, gd, rn = pl.pallas_call(
        functools.partial(kernel, fs, chunk),
        out_shape=(
            jax.ShapeDtypeStruct((tokens, ff), bf16),
            jax.ShapeDtypeStruct((tokens, ff), bf16),
            jax.ShapeDtypeStruct((8, ff), f32),
            jax.ShapeDtypeStruct((ff, dc), f32),
            jax.ShapeDtypeStruct((1, ff), f32),
        ),
        in_specs=[vmem] * 8,
        out_specs=(vmem,) * 5,
        scratch_shapes=[
            pltpu.VMEM((fs, ff, dc), bf16),
            pltpu.VMEM((fs, ff, dc), bf16),
            pltpu.VMEM((fs, ff, dc), bf16),
            pltpu.VMEM((ff, dc), f32),
            pltpu.VMEM((ff, dc), f32),
            pltpu.VMEM((fs, 8, ff), f32),
            pltpu.VMEM((8, ff), f32),
            pltpu.VMEM((8, ff), f32),
            pltpu.VMEM((fs, 1, ff), f32),
            dma((fs,)), dma((fs,)), dma((fs,)), dma((fs,)),
            dma((chunks, fs)), dma((chunks, fs)), dma((chunks,)), dma((chunks,)),
            dma((fs,)), dma((fs,)), dma, dma, dma((fs,)), dma((fs,)),
        ],
        compiler_params=pltpu.CompilerParams(
            collective_id=0, has_side_effects=True, vmem_limit_bytes=67043328),
    )(pre_gate, pre_linear, taps_gate, taps_linear, bias_gate[None], bias_linear[None],
      down_weight, out_grad)
    return gg, gl, cp[0:3], cp[3:6], cp[6], cp[7], gd, rn[0]


def solution(mesh):
    in_specs = (
        P(("rep", "fs"), "tp"),
        P(("rep", "fs"), "tp"),
        P(None, "tp"),
        P(None, "tp"),
        P("tp"),
        P("tp"),
        P("tp", "fs"),
        P(("rep", "fs"), None),
    )
    out_specs = (
        P(("rep", "fs"), "tp"),
        P(("rep", "fs"), "tp"),
        P(None, "tp"),
        P(None, "tp"),
        P("tp"),
        P("tp"),
        P("tp", "fs"),
        P("tp"),
    )
    return jax.shard_map(
        functools.partial(local, mesh.shape["fs"]), mesh=mesh, in_specs=in_specs, out_specs=out_specs, check_vma=False)
```

```python
import functools

import jax
import jax.numpy as jnp
from jax import lax
from jax.experimental import pallas as pl
from jax.experimental.pallas import tpu as pltpu
from jax.sharding import PartitionSpec as P

MESH = pl.DeviceIdType.MESH


def shift_down(values, steps):
    if steps == 0:
        return values
    rows = lax.broadcasted_iota(jnp.int32, values.shape, 0)
    return jnp.where(rows < steps, 0.0, pltpu.roll(values, steps, 0))


def shift_up(values, steps):
    length = values.shape[0]
    rows = lax.broadcasted_iota(jnp.int32, values.shape, 0)
    return jnp.where(rows >= length - steps, 0.0, pltpu.roll(values, length - steps, 0))


def conv_chunk(values, taps, bias):
    return (
        taps[0:1] * shift_down(values, 2)
        + taps[1:2] * shift_down(values, 1)
        + taps[2:3] * values
        + bias
    )


def conv_back_chunk(grads, taps):
    return taps[0:1] * shift_up(grads, 2) + taps[1:2] * shift_up(grads, 1) + taps[2:3] * grads


def kernel(
    fs, chunk,
    pg_ref, pl_ref, tg_ref, tl_ref, bg_ref, bl_ref, w_ref, og_ref,
    gg_ref, gl_ref, cp_ref, gd_ref, rn_ref,
    wbuf, sbuf, pbuf, rbuf, xs, xr, cpbuf, cps, cpx, rnbuf,
    w_send, w_recv, y_send, y_recv, p_send, p_recv, f_send, f_recv, s_send, s_recv, x_send, x_recv,
    c_send, c_recv, cx_send, cx_recv, n_send, n_recv,
):
    me = lax.axis_index("fs")
    rep = lax.axis_index("rep")
    partner = 1 - rep
    pairs = fs // 2
    z = me // 2
    par = me % 2
    mate = me + 1 - 2 * par
    tokens, ff = pg_ref.shape
    dc = w_ref.shape[1]
    chunks = ff // chunk
    half = ff // 2
    lag = chunks // 2
    per = -(-(fs - 1) // chunks)

    def to(k):
        return lax.rem(me + k, fs)

    def rows_of(c):
        return pl.ds(pl.multiple_of(c * chunk, chunk), chunk)

    def shard(z_at, parity):
        return z_at * 2 + parity

    def z_to(k):
        return lax.rem(z + k, pairs)

    def z_from(k):
        return lax.rem(z + pairs - k, pairs)

    def my_half():
        return pl.ds(pl.multiple_of(rep * half, half), half)

    def w_copy(k):
        return pltpu.make_async_remote_copy(
            src_ref=w_ref.at[my_half()], dst_ref=wbuf.at[me, my_half()],
            send_sem=w_send.at[k], recv_sem=w_recv.at[k],
            device_id={"fs": shard(z_to(k), par)}, device_id_type=MESH)

    def y_first():
        return pltpu.make_async_remote_copy(
            src_ref=w_ref.at[my_half()], dst_ref=wbuf.at[me, my_half()],
            send_sem=y_send.at[0], recv_sem=y_recv.at[0],
            device_id={"fs": mate}, device_id_type=MESH)

    def y_copy(k):
        block = wbuf.at[shard(z_from(k), par), my_half()]
        return pltpu.make_async_remote_copy(
            src_ref=block, dst_ref=block,
            send_sem=y_send.at[k], recv_sem=y_recv.at[k],
            device_id={"fs": mate}, device_id_type=MESH)

    def f_copy(item):
        block = wbuf.at[shard(z_from(item % pairs), (par + item // pairs) % 2), my_half()]
        return pltpu.make_async_remote_copy(
            src_ref=block, dst_ref=block,
            send_sem=f_send.at[item], recv_sem=f_recv.at[item],
            device_id={"rep": partner}, device_id_type=MESH)

    def p_copy(c):
        return pltpu.make_async_remote_copy(
            src_ref=sbuf.at[1 - par, :, rows_of(c)], dst_ref=pbuf.at[:, rows_of(c)],
            send_sem=p_send.at[c], recv_sem=p_recv.at[c],
            device_id={"fs": mate}, device_id_type=MESH)

    def s_copy(c, k):
        return pltpu.make_async_remote_copy(
            src_ref=sbuf.at[par, z_to(k), rows_of(c)], dst_ref=rbuf.at[k, rows_of(c)],
            send_sem=s_send.at[c, k], recv_sem=s_recv.at[c, k],
            device_id={"fs": shard(z_to(k), par)}, device_id_type=MESH)

    def pair_sum(c):
        p_copy(c).wait_recv()
        for at in range(pairs):
            both = sbuf[par, at, rows_of(c)].astype(jnp.float32) + pbuf[at, rows_of(c)].astype(jnp.float32)
            sbuf[par, at, rows_of(c)] = both.astype(jnp.bfloat16)

        @pl.loop(1, pairs)
        def _(k):
            s_copy(c, k).start()

    def x_copy(c):
        return pltpu.make_async_remote_copy(
            src_ref=xs.at[rows_of(c)], dst_ref=xr.at[rows_of(c)],
            send_sem=x_send.at[c], recv_sem=x_recv.at[c],
            device_id={"rep": partner}, device_id_type=MESH)

    def c_copy(k):
        return pltpu.make_async_remote_copy(
            src_ref=cpbuf.at[me], dst_ref=cpbuf.at[me],
            send_sem=c_send.at[k], recv_sem=c_recv.at[k],
            device_id={"fs": to(k)}, device_id_type=MESH)

    def cx_copy():
        return pltpu.make_async_remote_copy(
            src_ref=cps, dst_ref=cpx, send_sem=cx_send, recv_sem=cx_recv,
            device_id={"rep": partner}, device_id_type=MESH)

    def n_copy(k):
        return pltpu.make_async_remote_copy(
            src_ref=rnbuf.at[me], dst_ref=rnbuf.at[me],
            send_sem=n_send.at[k], recv_sem=n_recv.at[k],
            device_id={"fs": to(k)}, device_id_type=MESH)

    barrier = pltpu.get_barrier_semaphore()

    @pl.loop(1, fs)
    def _(k):
        pl.semaphore_signal(barrier, inc=1, device_id={"fs": to(k)}, device_id_type=MESH)

    pl.semaphore_signal(barrier, inc=1, device_id={"rep": partner}, device_id_type=MESH)
    pl.semaphore_wait(barrier, fs)

    y_first().start()

    @pl.loop(1, pairs)
    def _(k):
        w_copy(k).start()

    wbuf[me] = w_ref[...]

    @pl.loop(0, chunks)
    def _(c):
        cols = rows_of(c)
        gate_pre = conv_chunk(
            pg_ref[:, cols].astype(jnp.float32), tg_ref[:, cols], bg_ref[:, cols])
        linear_pre = conv_chunk(
            pl_ref[:, cols].astype(jnp.float32), tl_ref[:, cols], bl_ref[:, cols])
        hidden = (gate_pre * jax.nn.sigmoid(gate_pre) * linear_pre).astype(jnp.bfloat16)
        for j in range(fs):
            part = lax.dot_general(
                hidden, og_ref[:, j * dc:(j + 1) * dc], (((0,), (0,)), ((), ())),
                preferred_element_type=jnp.float32)
            sbuf[j % 2, j // 2, cols] = part.astype(jnp.bfloat16)

        p_copy(c).start()

        @pl.when(c >= lag)
        def _():
            pair_sum(c - lag)

        for step in range(per):
            k = c * per + step + 1

            @pl.when(k < pairs)
            def _():
                w_copy(k).wait_recv()
                y_copy(k).start()
                f_copy(k).start()

            @pl.when((k >= pairs) & (k < fs))
            def _():
                y_copy(k - pairs).wait_recv()
                f_copy(k).start()

    @pl.loop(1, fs)
    def _(k):
        f_copy(k).wait_recv()

    @pl.loop(0, chunks)
    def _(c):
        cols = rows_of(c)
        gate_in = pg_ref[:, cols].astype(jnp.float32)
        linear_in = pl_ref[:, cols].astype(jnp.float32)
        taps_gate, taps_linear = tg_ref[:, cols], tl_ref[:, cols]
        gate_pre = conv_chunk(gate_in, taps_gate, bg_ref[:, cols])
        linear_pre = conv_chunk(linear_in, taps_linear, bl_ref[:, cols])
        sigma = jax.nn.sigmoid(gate_pre)
        grad_hidden = jnp.zeros((tokens, chunk), jnp.float32)
        for j in range(fs):
            grad_hidden += lax.dot_general(
                og_ref[:, j * dc:(j + 1) * dc], wbuf[j, cols], (((1,), (1,)), ((), ())),
                preferred_element_type=jnp.float32)
        grad_gate_pre = grad_hidden * linear_pre * sigma * (1.0 + gate_pre * (1.0 - sigma))
        grad_linear_pre = grad_hidden * (gate_pre * sigma)
        gg_ref[:, cols] = conv_back_chunk(grad_gate_pre, taps_gate).astype(jnp.bfloat16)
        gl_ref[:, cols] = conv_back_chunk(grad_linear_pre, taps_linear).astype(jnp.bfloat16)
        for j in range(3):
            cpbuf[me, j:j + 1, cols] = jnp.sum(
                grad_gate_pre * shift_down(gate_in, 2 - j), axis=0, keepdims=True)
            cpbuf[me, j + 3:j + 4, cols] = jnp.sum(
                grad_linear_pre * shift_down(linear_in, 2 - j), axis=0, keepdims=True)
        cpbuf[me, 6:7, cols] = jnp.sum(grad_gate_pre, axis=0, keepdims=True)
        cpbuf[me, 7:8, cols] = jnp.sum(grad_linear_pre, axis=0, keepdims=True)

        @pl.when(c == chunks - 1)
        def _():
            @pl.loop(1, fs)
            def _(k):
                c_copy(k).start()

        @pl.when(c < lag)
        def _():
            pair_sum(chunks - lag + c)

        total = sbuf[par, z, cols].astype(jnp.float32)
        for k in range(1, pairs):
            s_copy(c, k).wait_recv()
            total += rbuf[k, cols].astype(jnp.float32)
        xs[cols] = total
        x_copy(c).start()

    @pl.loop(1, fs)
    def _(k):
        c_copy(k).wait_recv()

    sums = cpbuf[0]
    for j in range(1, fs):
        sums += cpbuf[j]
    cps[...] = sums
    cx_copy().start()

    @pl.loop(0, chunks)
    def _(c):
        rows = rows_of(c)
        x_copy(c).wait_recv()
        total = xs[rows] + xr[rows]
        gd_ref[rows] = total
        square = total * total
        while square.shape[1] % 256 == 0:
            middle = square.shape[1] // 2
            square = square[:, :middle] + square[:, middle:]
        rnbuf[me, 0:1, rows] = jnp.sum(square.T, axis=0, keepdims=True)

    @pl.loop(1, fs)
    def _(k):
        n_copy(k).start()

    cx_copy().wait_recv()
    cp_ref[...] = cps[...] + cpx[...]

    @pl.loop(1, fs)
    def _(k):
        n_copy(k).wait_recv()

    norms = rnbuf[0]
    for j in range(1, fs):
        norms += rnbuf[j]
    rn_ref[...] = norms

    cx_copy().wait_send()
    y_first().wait_send()

    @pl.loop(1, pairs)
    def _(k):
        w_copy(k).wait_send()
        y_copy(k).wait_send()

    @pl.loop(1, fs)
    def _(k):
        f_copy(k).wait_send()
        c_copy(k).wait_send()
        n_copy(k).wait_send()

    @pl.loop(0, chunks)
    def _(c):
        x_copy(c).wait_send()
        p_copy(c).wait_send()

        @pl.loop(1, pairs)
        def _(k):
            s_copy(c, k).wait_send()


def local(
    fs, pre_gate, pre_linear, taps_gate, taps_linear, bias_gate, bias_linear, down_weight, out_grad
):
    tokens, ff = pre_gate.shape
    dc = down_weight.shape[1]
    chunk = 256
    chunks = ff // chunk
    pairs = fs // 2
    f32, bf16 = jnp.float32, jnp.bfloat16
    vmem = pl.BlockSpec(memory_space=pltpu.VMEM)
    dma = pltpu.SemaphoreType.DMA
    gg, gl, cp, gd, rn = pl.pallas_call(
        functools.partial(kernel, fs, chunk),
        out_shape=(
            jax.ShapeDtypeStruct((tokens, ff), bf16),
            jax.ShapeDtypeStruct((tokens, ff), bf16),
            jax.ShapeDtypeStruct((8, ff), f32),
            jax.ShapeDtypeStruct((ff, dc), f32),
            jax.ShapeDtypeStruct((1, ff), f32),
        ),
        in_specs=[vmem] * 8,
        out_specs=(vmem,) * 5,
        scratch_shapes=[
            pltpu.VMEM((fs, ff, dc), bf16),
            pltpu.VMEM((2, pairs, ff, dc), bf16),
            pltpu.VMEM((pairs, ff, dc), bf16),
            pltpu.VMEM((pairs, ff, dc), bf16),
            pltpu.VMEM((ff, dc), f32),
            pltpu.VMEM((ff, dc), f32),
            pltpu.VMEM((fs, 8, ff), f32),
            pltpu.VMEM((8, ff), f32),
            pltpu.VMEM((8, ff), f32),
            pltpu.VMEM((fs, 1, ff), f32),
            dma((pairs,)), dma((pairs,)), dma((pairs,)), dma((pairs,)),
            dma((chunks,)), dma((chunks,)), dma((fs,)), dma((fs,)),
            dma((chunks, pairs)), dma((chunks, pairs)), dma((chunks,)), dma((chunks,)),
            dma((fs,)), dma((fs,)), dma, dma, dma((fs,)), dma((fs,)),
        ],
        compiler_params=pltpu.CompilerParams(
            collective_id=0, has_side_effects=True, vmem_limit_bytes=67043328),
    )(pre_gate, pre_linear, taps_gate, taps_linear, bias_gate[None], bias_linear[None],
      down_weight, out_grad)
    return gg, gl, cp[0:3], cp[3:6], cp[6], cp[7], gd, rn[0]


def solution(mesh):
    in_specs = (
        P(("rep", "fs"), "tp"),
        P(("rep", "fs"), "tp"),
        P(None, "tp"),
        P(None, "tp"),
        P("tp"),
        P("tp"),
        P("tp", "fs"),
        P(("rep", "fs"), None),
    )
    out_specs = (
        P(("rep", "fs"), "tp"),
        P(("rep", "fs"), "tp"),
        P(None, "tp"),
        P(None, "tp"),
        P("tp"),
        P("tp"),
        P("tp", "fs"),
        P("tp"),
    )
    return jax.shard_map(
        functools.partial(local, mesh.shape["fs"]), mesh=mesh, in_specs=in_specs, out_specs=out_specs, check_vma=False)
```
